32 devices in a mesh: sp: 8 (over z, y), dp: 4 (over x, core).
Axes of the slice: x: 2, y: 2, z: 4, core: 2. Of those that a mesh axis runs over, the one named last changes fastest.
Arguments:
- queries: bfloat16 [4, 1024, 16, 128], P('dp', 'sp'), may hold values from -7 to 7
- key_vectors: bfloat16 [4, 1024, 16, 128], P('dp', 'sp'), may hold values from -6 to 6
- value_vectors: bfloat16 [4, 1024, 16, 128], P('dp', 'sp'), may hold values from -6 to 6
- head_lambda: float32 [16], P('sp'), may hold values from 0.3 to 0.8
- head_gain: float32 [128], replicated, may hold values from 0.1 to 1.9
- residual: bfloat16 [4, 1024, 2048], P('dp', 'sp'), may hold values from -6 to 6
- out_weight: bfloat16 [2048, 2048], replicated, may hold values from -0.125 to 0.125
- mix_gain: float32 [2048], replicated, may hold values from 0.1 to 1.9
- pre_gain: float32 [2048], replicated, may hold values from 0.1 to 1.9
- post_gain: float32 [2048], replicated, may hold values from 0.1 to 1.9
- routes: int32 [4, 1024, 4], P('dp', 'sp'), may hold values from 0 to 31, all different within a row; in each aligned block of 128 rows (0 to 127, 128 to 255, ..., all dimensions but the last counted through in order) at most 24 rows name the same one
- route_weights: float32 [4, 1024, 4], P('dp', 'sp'), may hold values from 0.25 to 1
- expert_gate: bfloat16 [32, 2048, 512], P(('sp', 'dp')), may hold values from -0.125 to 0.125
- expert_up: bfloat16 [32, 2048, 512], P(('sp', 'dp')), may hold values from -0.125 to 0.125
- expert_down: bfloat16 [32, 512, 2048], P(('sp', 'dp')), may hold values from -0.25 to 0.25
- shared_gate: bfloat16 [2048, 512], replicated, may hold values from -0.125 to 0.125
- shared_up: bfloat16 [2048, 512], replicated, may hold values from -0.125 to 0.125
- shared_down: bfloat16 [512, 2048], replicated, may hold values from -0.25 to 0.25
Outputs:
- output: bfloat16 [4, 1024, 2048], P('dp', 'sp')
The draws below stay inside these ranges and needn't reach their ends.
Inputs may be any that keep to these rules, and one draw needn't show every extreme that they name: `routes`: among the tokens of one device (aligned blocks of 128 positions), no expert is named more than 24 times; in some block some expert is named exactly 24 times. Each token names 4 different experts.
All inputs are finite; a program needn't handle non-finite values.
Results may differ from the reference program's by a relative error of at most 0.0075.
Values may be sent and summed in bfloat16 or wider, within the bound.
A program may use at most 128 MiB of HBM per device.

```python
import math
import jax
import jax.numpy as jnp
import numpy as np
from jax import lax

D = 2048
HEADS = 16
HD = 64
VD = 128
FF = 512
TOP_K = 4
TOK_DEV = 128
LEN = 1024
SEQS = 4
EXPERTS = 32
CAP = 24


def draw_queries(key, part):
    shape = (SEQS, LEN, HEADS, 2 * HD)
    base_key = jax.random.fold_in(key, 11)
    drawn = jnp.clip(1.75 * jax.random.normal(base_key, shape, jnp.float32), -7.0, 7.0)
    return drawn.astype(jnp.bfloat16)


def draw_key_vectors(key, part):
    shape = (SEQS, LEN, HEADS, 2 * HD)
    base_key = jax.random.fold_in(key, 13)
    drawn = jnp.clip(jax.random.normal(base_key, shape, jnp.float32), -6.0, 6.0)
    return drawn.astype(jnp.bfloat16)


def levels(key, dims, cuts, least, top_value):
    def one(position, parts):
        draws = jax.random.uniform(jax.random.fold_in(jax.random.fold_in(key, 6), position), (parts,), jnp.float32, least / len(cuts), top_value / len(cuts))
        return jnp.repeat(jnp.exp(draws), dims[position] // parts).reshape((-1,) + (1,) * (len(dims) - position - 1))

    level = one(*cuts[0])
    for cut in cuts[1:]:
        level = level * one(*cut)
    return level


def deal_out(rng, own, number, rows, amount, top, reach, slope):
    sequence = jax.random.permutation(rng, amount)
    heavy_load, common = portions_of(amount, rows * top, reach, slope, True), portions_of(amount, rows * top, reach, slope, False)
    places = jnp.arange(amount)

    def named(lengths, rotation):
        used = int((lengths > 0).sum())
        fixed = max(1, used // 4)
        passed = fixed + (places - fixed + rotation * (used - fixed)) % max(1, amount - fixed)
        return jnp.zeros((amount,), jnp.int32).at[sequence[jnp.where(places < fixed, places, passed)]].set(jnp.asarray(lengths, jnp.int32))

    lengths = jnp.where(number % 4 == 0, named(heavy_load, number // 4), named(common, number - number // 4 - 1))
    mixed = jax.random.permutation(jax.random.fold_in(own, 3), amount)
    source_of, sink = mixed[0:amount // 2 * 2:2], mixed[1:amount // 2 * 2:2]
    room = jnp.minimum(lengths[source_of] - 1, reach - lengths[sink]) // 2
    room = jnp.where((source_of == sequence[0]) | (sink == sequence[0]) | (lengths[sink] == 0), 0, jnp.maximum(room, 0))
    passed = jax.random.randint(jax.random.fold_in(own, 4), (amount // 2,), 0, 1 << 20) % (room + 1)
    lengths = lengths.at[source_of].add(-passed).at[sink].add(passed)
    members = jnp.searchsorted(jnp.cumsum(lengths), jnp.arange(rows * top), side="right").astype(jnp.int32)
    listing = members.reshape(top, rows).T
    listing = listing[jax.random.permutation(jax.random.fold_in(own, 1), rows)]
    rotation = jax.random.randint(jax.random.fold_in(own, 2), (rows, 1), 0, top)
    return jnp.take_along_axis(listing, (jnp.arange(top)[None, :] + rotation) % top, axis=1)


def portions_of(count, total, reach, lean, full):
    weights = [(1 << 20) // math.isqrt(grade ** lean) + 1 for grade in range(1, count + 1)]
    largest = reach if full else min(reach, max(-(-total // count), total * weights[0] // sum(weights)))
    least = 1 if total - largest >= count - 1 else 0
    counts, spare = [largest] + [least] * (count - 1), total - largest - least * (count - 1)
    while spare > 0:
        candidates = [i for i in range(1, count) if counts[i] < largest] or [i for i in range(1, count) if counts[i] < reach]
        whole, remaining = sum([weights[i] for i in candidates]), spare
        for i in candidates:
            extra = min(reach - counts[i], max(1, remaining * weights[i] // whole), spare)
            counts[i] = counts[i] + extra
            spare = spare - extra
    return np.array(counts)


def bell_draw(rng, dims, spread, reach, pieces=(), held_as=jnp.bfloat16):
    values = spread * jax.random.normal(rng, dims, jnp.float32)
    if pieces:
        values = values * levels(rng, dims, pieces, -0.22, 0.18)
    return jnp.clip(values, -reach, reach).astype(held_as)


def setup_inputs(seed: int = 0) -> dict:
    key_list = jax.random.split(jax.random.key(seed), 19)
    queries = draw_queries(jax.random.fold_in(key_list[18], 71), 0)
    key_vectors = draw_key_vectors(jax.random.fold_in(key_list[18], 71), 0)
    value_vectors = bell_draw(key_list[2], (SEQS, LEN, HEADS, VD), 1.0, 6.0, ((0, 4), (1, 8)))
    head_lambda = jnp.clip(0.3 + 0.5 * jax.random.uniform(key_list[3], (HEADS,), jnp.float32) ** levels(key_list[3], (HEADS,), ((0, 8),), -0.2, 0.2), 0.3, 0.8)
    head_gain = jnp.clip(1.0 + 0.18 * jax.random.normal(key_list[4], (VD,), jnp.float32), 0.1, 1.9)
    residual = bell_draw(key_list[5], (SEQS, LEN, D), 1.0, 6.0, ((0, 4), (1, 8)))
    out_weight = bell_draw(key_list[6], (HEADS * VD, D), (HEADS * VD) ** -0.5, 0.125)
    mix_gain = jnp.clip(1.0 + 0.18 * jax.random.normal(key_list[7], (D,), jnp.float32), 0.1, 1.9)
    pre_gain = jnp.clip(1.0 + 0.18 * jax.random.normal(key_list[8], (D,), jnp.float32), 0.1, 1.9)
    post_gain = jnp.clip(1.0 + 0.18 * jax.random.normal(key_list[9], (D,), jnp.float32), 0.1, 1.9)
    routes_keys = jax.random.split(jax.random.fold_in(key_list[10], 1), SEQS * LEN // TOK_DEV)
    routes_turns = jax.random.permutation(jax.random.fold_in(key_list[10], 3), SEQS * LEN // TOK_DEV)
    routes = jax.vmap(lambda own, number: deal_out(jax.random.fold_in(key_list[10], 2), own, number, TOK_DEV, EXPERTS, TOP_K, CAP, 2))(routes_keys, routes_turns).reshape((SEQS, LEN, TOP_K))
    route_weights = jnp.clip(0.25 + 0.75 * jax.random.uniform(key_list[11], (SEQS, LEN, TOP_K), jnp.float32) ** levels(key_list[11], (SEQS, LEN, TOP_K), ((0, 4), (1, 8)), -0.2, 0.2), 0.25, 1.0)
    expert_gate = bell_draw(key_list[12], (EXPERTS, D, FF), D ** -0.5, 0.125, ((0, 32),))
    expert_up = bell_draw(key_list[13], (EXPERTS, D, FF), D ** -0.5, 0.125, ((0, 32),))
    expert_down = bell_draw(key_list[14], (EXPERTS, FF, D), FF ** -0.5, 0.25, ((0, 32),))
    shared_gate = bell_draw(key_list[15], (D, FF), D ** -0.5, 0.125)
    shared_up = bell_draw(key_list[16], (D, FF), D ** -0.5, 0.125)
    shared_down = bell_draw(key_list[17], (FF, D), FF ** -0.5, 0.25)
    return dict(queries=queries, key_vectors=key_vectors, value_vectors=value_vectors, head_lambda=head_lambda, head_gain=head_gain, residual=residual, out_weight=out_weight, mix_gain=mix_gain, pre_gain=pre_gain, post_gain=post_gain, routes=routes, route_weights=route_weights, expert_gate=expert_gate, expert_up=expert_up, expert_down=expert_down, shared_gate=shared_gate, shared_up=shared_up, shared_down=shared_down)


epsilon = 1e-06

def rms_scale(values_in, gain):
    return values_in * lax.rsqrt(lax.optimization_barrier(jnp.mean(values_in * values_in, axis=-1, keepdims=True)) + epsilon) * gain

def feed_forward(rows, gate_w, up_w, down_w):
    gate_val = jnp.dot(rows, gate_w, preferred_element_type=jnp.float32)
    up_val = jnp.dot(rows, up_w, preferred_element_type=jnp.float32)
    hidden = (jax.nn.silu(gate_val) * up_val).astype(jnp.bfloat16)
    return jnp.dot(hidden, down_w, preferred_element_type=jnp.float32).astype(jnp.bfloat16)

def attend_sequence(query_seq, key_seq, value_seq, head_lambda, head_gain):
    length = query_seq.shape[0]
    head_count = query_seq.shape[1]
    head_size = query_seq.shape[2] // 2
    block_rows = min(512, length)
    block_count = length // block_rows
    query_blocks = query_seq.astype(jnp.float32).reshape(block_count, block_rows, head_count, 2, head_size)
    key_all = key_seq.astype(jnp.float32).reshape(length, head_count, 2, head_size)
    value_all = value_seq.astype(jnp.float32)
    key_pos = jnp.arange(length, dtype=jnp.int32)

    def one_block(inputs):
        query_block, block_index = inputs
        scores = jnp.einsum('qhmd,khmd->hmqk', query_block, key_all) * head_size ** (-0.5)
        query_pos = block_index * block_rows + jnp.arange(block_rows, dtype=jnp.int32)
        causal = key_pos[None, :] <= query_pos[:, None]
        scores = jnp.where(causal, scores, -jnp.inf)
        maxima = lax.optimization_barrier(jnp.max(scores, axis=-1, keepdims=True))
        exponent = jnp.exp(scores - maxima)
        softmax_both = exponent / lax.optimization_barrier(jnp.sum(exponent, axis=-1, keepdims=True))
        mixture = softmax_both[:, 0] - head_lambda[:, None, None] * softmax_both[:, 1]
        mixture_low = lax.optimization_barrier(mixture.astype(jnp.bfloat16)).astype(jnp.float32)
        head_output = jnp.einsum('hqk,khe->qhe', mixture_low, value_all)
        return rms_scale(head_output, head_gain).astype(jnp.bfloat16)
    outputs = lax.map(one_block, (query_blocks, jnp.arange(block_count, dtype=jnp.int32)))
    return outputs.reshape(length, head_count, -1)

def reference(queries, key_vectors, value_vectors, head_lambda, head_gain, residual, out_weight, mix_gain, pre_gain, post_gain, routes, route_weights, expert_gate, expert_up, expert_down, shared_gate, shared_up, shared_down):
    heads_out = lax.map(lambda inputs: attend_sequence(inputs[0], inputs[1], inputs[2], head_lambda, head_gain), (queries, key_vectors, value_vectors))
    token_total = SEQS * LEN
    flat_heads = heads_out.reshape(token_total, HEADS * VD)
    mixed_rows = jnp.dot(flat_heads, out_weight, preferred_element_type=jnp.float32)
    updated = (residual.reshape(token_total, D).astype(jnp.float32) + rms_scale(mixed_rows, mix_gain)).astype(jnp.bfloat16)
    normed = rms_scale(updated.astype(jnp.float32), pre_gain).astype(jnp.bfloat16)
    shared_out = feed_forward(normed, shared_gate, shared_up, shared_down)
    block_total = token_total // TOK_DEV
    assign_block = TOK_DEV * TOP_K
    flat_routes = routes.reshape(block_total, assign_block).astype(jnp.int32)
    one_hot = (flat_routes[:, :, None] == jnp.arange(EXPERTS, dtype=jnp.int32)[None, None, :]).astype(jnp.int32)
    earlier = jnp.cumsum(one_hot, axis=1) - one_hot
    rank_index = lax.optimization_barrier(jnp.sum(earlier * one_hot, axis=2))
    block_ids = jnp.arange(block_total, dtype=jnp.int32)[:, None]
    slot_index = (flat_routes * (block_total * CAP) + block_ids * CAP + rank_index).reshape(-1)
    assign_ids = jnp.arange(block_total * assign_block, dtype=jnp.int32)
    source_table = jnp.zeros((EXPERTS * block_total * CAP,), jnp.int32).at[slot_index].set(assign_ids)
    rows_per_expert = source_table.reshape(EXPERTS, block_total * CAP) // TOP_K

    def run_expert(inputs):
        row_ids, gate_w, up_w, down_w = inputs
        return feed_forward(normed[row_ids], gate_w, up_w, down_w)
    expert_out = lax.map(run_expert, (rows_per_expert, expert_gate, expert_up, expert_down))
    picked = expert_out.reshape(EXPERTS * block_total * CAP, D)[slot_index]
    routed = lax.optimization_barrier(jnp.sum(picked.astype(jnp.float32).reshape(token_total, TOP_K, D) * route_weights.reshape(token_total, TOP_K, 1), axis=1))
    combined = routed + shared_out.astype(jnp.float32)
    output = (updated.astype(jnp.float32) + rms_scale(combined, post_gain)).astype(jnp.bfloat16)
    return output.reshape(SEQS, LEN, D)
```

```python
import functools

import jax
import jax.numpy as jnp
from jax import lax
from jax.experimental import pallas as pl
from jax.experimental.pallas import tpu as pltpu
from jax.sharding import PartitionSpec as P

epsilon = 1e-06
MESH = pl.DeviceIdType.MESH
VMEM = pl.BlockSpec(memory_space=pltpu.VMEM)


def rms_scale(values_in, gain):
    return (
        values_in
        * lax.rsqrt(jnp.mean(values_in * values_in, axis=-1, keepdims=True) + epsilon)
        * gain
    )


def feed_forward(rows, gate_w, up_w, down_w):
    gate_val = jnp.dot(rows, gate_w, preferred_element_type=jnp.float32)
    up_val = jnp.dot(rows, up_w, preferred_element_type=jnp.float32)
    hidden = (jax.nn.silu(gate_val) * up_val).astype(jnp.bfloat16)
    return jnp.dot(hidden, down_w, preferred_element_type=jnp.float32).astype(jnp.bfloat16)


def columns_of(index, width):
    return pl.ds(pl.multiple_of(index * width, width), width)


def line_barrier(n, me):
    barrier = pltpu.get_barrier_semaphore()

    def greet(off, carry):
        pl.semaphore_signal(
            barrier, inc=1, device_id={"sp": lax.rem(me + off, n)}, device_id_type=MESH
        )
        return carry

    lax.fori_loop(1, n, greet, 0)
    pl.semaphore_wait(barrier, n - 1)


def to_heads_kernel(n, q_ref, k_ref, v_ref, qo_ref, ko_ref, vo_ref, send_sem, recv_sem, own_sem):
    me = lax.axis_index("sp")
    width = qo_ref.shape[2]
    pairs = ((q_ref, qo_ref), (k_ref, ko_ref), (v_ref, vo_ref))
    line_barrier(n, me)

    def copy(which, off):
        source, target = pairs[which]
        dst = lax.rem(me + off, n)
        return pltpu.make_async_remote_copy(
            src_ref=source.at[:, columns_of(dst, width)],
            dst_ref=target.at[me],
            send_sem=send_sem.at[which, off],
            recv_sem=recv_sem.at[which, off],
            device_id={"sp": dst},
            device_id_type=MESH,
        )

    def own(which):
        source, target = pairs[which]
        return pltpu.make_async_copy(
            source.at[:, columns_of(me, width)], target.at[me], own_sem.at[which]
        )

    def start(off, carry):
        for which in range(3):
            copy(which, off).start()
        return carry

    def finish(off, carry):
        for which in range(3):
            copy(which, off).wait()
        return carry

    lax.fori_loop(1, n, start, 0)
    for which in range(3):
        own(which).start()
    for which in range(3):
        own(which).wait()
    lax.fori_loop(1, n, finish, 0)


def to_heads(n, q, k, v):
    tok, model = q.shape
    width = model // n
    out = jax.ShapeDtypeStruct((n, tok, width), q.dtype)
    return pl.pallas_call(
        functools.partial(to_heads_kernel, n),
        out_shape=[out] * 3,
        in_specs=[VMEM] * 3,
        out_specs=[VMEM] * 3,
        scratch_shapes=[
            pltpu.SemaphoreType.DMA((3, n)),
            pltpu.SemaphoreType.DMA((3, n)),
            pltpu.SemaphoreType.DMA((3,)),
        ],
        compiler_params=pltpu.CompilerParams(
            collective_id=0, has_side_effects=True, vmem_limit_bytes=32 * 2**20
        ),
    )(q, k, v)


def to_tokens_kernel(n, a_ref, o_ref, send_sem, recv_sem, own_sem):
    me = lax.axis_index("sp")
    width = a_ref.shape[2]
    line_barrier(n, me)

    def copy(off):
        dst = lax.rem(me + off, n)
        return pltpu.make_async_remote_copy(
            src_ref=a_ref.at[dst],
            dst_ref=o_ref.at[:, columns_of(me, width)],
            send_sem=send_sem.at[off],
            recv_sem=recv_sem.at[off],
            device_id={"sp": dst},
            device_id_type=MESH,
        )

    def start(off, carry):
        copy(off).start()
        return carry

    def finish(off, carry):
        copy(off).wait()
        return carry

    lax.fori_loop(1, n, start, 0)
    own = pltpu.make_async_copy(a_ref.at[me], o_ref.at[:, columns_of(me, width)], own_sem)
    own.start()
    own.wait()
    lax.fori_loop(1, n, finish, 0)


def to_tokens(n, attended):
    _, tok, width = attended.shape
    return pl.pallas_call(
        functools.partial(to_tokens_kernel, n),
        out_shape=jax.ShapeDtypeStruct((tok, n * width), attended.dtype),
        in_specs=[VMEM],
        out_specs=VMEM,
        scratch_shapes=[
            pltpu.SemaphoreType.DMA((n,)),
            pltpu.SemaphoreType.DMA((n,)),
            pltpu.SemaphoreType.DMA,
        ],
        compiler_params=pltpu.CompilerParams(
            collective_id=1, has_side_effects=True, vmem_limit_bytes=32 * 2**20
        ),
    )(attended)


def attend_kernel(block, q_ref, k_ref, v_ref, lam_ref, gain_ref, o_ref):
    length, width = q_ref.shape
    value_size = gain_ref.shape[1]
    heads = width // value_size
    half = value_size // 2
    lane = lax.broadcasted_iota(jnp.int32, (block, value_size), 1)
    row = lax.broadcasted_iota(jnp.int32, (block, block), 0)
    col = lax.broadcasted_iota(jnp.int32, (block, block), 1)
    causal = col <= row
    contract = (((1,), (1,)), ((), ()))
    for head in range(heads):
        cols = slice(head * value_size, (head + 1) * value_size)
        for step in range(length // block):
            rows = slice(step * block, (step + 1) * block)
            past = step * block
            query = q_ref[rows, cols]
            near, far = [], []
            for which in range(2):
                keep = (lane < half) if which == 0 else (lane >= half)
                part = jnp.where(keep, query, jnp.zeros_like(query))
                s_near = lax.dot_general(
                    part, k_ref[rows, cols], contract, preferred_element_type=jnp.float32
                ) * (half**-0.5)
                s_near = jnp.where(causal, s_near, -jnp.inf)
                top = jnp.max(s_near, axis=-1, keepdims=True)
                if past:
                    s_far = lax.dot_general(
                        part, k_ref[:past, cols], contract, preferred_element_type=jnp.float32
                    ) * (half**-0.5)
                    top = jnp.maximum(top, jnp.max(s_far, axis=-1, keepdims=True))
                e_near = jnp.exp(s_near - top)
                total = jnp.sum(e_near, axis=-1, keepdims=True)
                if past:
                    e_far = jnp.exp(s_far - top)
                    total = total + jnp.sum(e_far, axis=-1, keepdims=True)
                scale = 1.0 / total
                if which == 1:
                    scale = scale * lam_ref[head]
                near.append(e_near * scale)
                if past:
                    far.append(e_far * scale)
            mixture = (near[0] - near[1]).astype(jnp.bfloat16)
            result = jnp.dot(mixture, v_ref[rows, cols], preferred_element_type=jnp.float32)
            if past:
                mixture = (far[0] - far[1]).astype(jnp.bfloat16)
                result += jnp.dot(
                    mixture, v_ref[:past, cols], preferred_element_type=jnp.float32
                )
            o_ref[rows, cols] = rms_scale(result, gain_ref[...]).astype(o_ref.dtype)


def attend(q, k, v, head_lambda, head_gain):
    return pl.pallas_call(
        functools.partial(attend_kernel, min(256, q.shape[0])),
        out_shape=jax.ShapeDtypeStruct(q.shape, q.dtype),
        in_specs=[VMEM] * 3 + [pl.BlockSpec(memory_space=pltpu.SMEM), VMEM],
        out_specs=VMEM,
        compiler_params=pltpu.CompilerParams(vmem_limit_bytes=48 * 2**20),
    )(q, k, v, head_lambda, head_gain.reshape(1, -1))


def half_place(sp_half, dp_size):
    sp, dp = lax.axis_index("sp"), lax.axis_index("dp")
    first = sp // sp_half * sp_half
    here = (sp - first) * dp_size + dp
    mirror = {"sp": lax.rem(sp + sp_half, 2 * sp_half), "dp": dp}

    def peer(place):
        return {"sp": first + place // dp_size, "dp": lax.rem(place, dp_size)}

    return here, mirror, peer


def half_barrier(group, here, mirror, peer):
    barrier = pltpu.get_barrier_semaphore()
    pl.semaphore_signal(barrier, inc=1, device_id=mirror, device_id_type=MESH)

    def greet(off, carry):
        pl.semaphore_signal(
            barrier, inc=1, device_id=peer(lax.rem(here + off, group)), device_id_type=MESH
        )
        return carry

    lax.fori_loop(1, group, greet, 0)
    pl.semaphore_wait(barrier, group)


def dispatch_kernel(
    sp_half,
    dp_size,
    own_ref,
    normed_ref,
    pick_ref,
    o_ref,
    tokens,
    rows,
    send_sem,
    recv_sem,
    far_send,
    far_recv,
    own_sem,
):
    group = sp_half * dp_size
    chunks, _, _, width = rows.shape
    here, mirror, peer = half_place(sp_half, dp_size)
    half_barrier(group, here, mirror, peer)

    def far(chunk):
        cols = pl.ds(chunk * width, width)
        return pltpu.make_async_remote_copy(
            src_ref=normed_ref.at[:, cols],
            dst_ref=tokens.at[chunk],
            send_sem=far_send.at[chunk],
            recv_sem=far_recv.at[chunk],
            device_id=mirror,
            device_id_type=MESH,
        )

    def near(off):
        place = lax.rem(here + off, group)
        return pltpu.make_async_remote_copy(
            src_ref=own_ref.at[place],
            dst_ref=o_ref.at[here],
            send_sem=send_sem.at[chunks, off],
            recv_sem=recv_sem.at[chunks, off],
            device_id=peer(place),
            device_id_type=MESH,
        )

    def passed(chunk, off):
        place = lax.rem(here + off, group)
        return pltpu.make_async_remote_copy(
            src_ref=rows.at[chunk, place],
            dst_ref=o_ref.at[group + here, :, pl.ds(chunk * width, width)],
            send_sem=send_sem.at[chunk, off],
            recv_sem=recv_sem.at[chunk, off],
            device_id=peer(place),
            device_id_type=MESH,
        )

    def over(action):
        lax.fori_loop(1, group, lambda off, carry: (action(off), carry)[1], 0)

    for chunk in range(chunks):
        far(chunk).start()
    over(lambda off: near(off).start())
    kept = pltpu.make_async_copy(own_ref.at[here], o_ref.at[here], own_sem.at[chunks])
    kept.start()
    for chunk in range(chunks):
        far(chunk).wait_recv()
        picked = jnp.dot(pick_ref[...], tokens[chunk], preferred_element_type=jnp.float32)
        rows[chunk] = picked.reshape(rows.shape[1:]).astype(rows.dtype)
        over(lambda off: passed(chunk, off).start())
        pltpu.make_async_copy(
            rows.at[chunk, here],
            o_ref.at[group + here, :, pl.ds(chunk * width, width)],
            own_sem.at[chunk],
        ).start()
    kept.wait()
    over(lambda off: near(off).wait())
    for chunk in range(chunks):
        far(chunk).wait_send()
        over(lambda off: passed(chunk, off).wait())
        pltpu.make_async_copy(
            rows.at[chunk, here],
            o_ref.at[group + here, :, pl.ds(chunk * width, width)],
            own_sem.at[chunk],
        ).wait()


def dispatch(sp_half, dp_size, own_rows, normed, pick_far, chunks):
    group, cap, model = own_rows.shape
    tok = normed.shape[0]
    width = model // chunks
    return pl.pallas_call(
        functools.partial(dispatch_kernel, sp_half, dp_size),
        out_shape=jax.ShapeDtypeStruct((2 * group, cap, model), normed.dtype),
        in_specs=[VMEM] * 3,
        out_specs=VMEM,
        scratch_shapes=[
            pltpu.VMEM((chunks, tok, width), normed.dtype),
            pltpu.VMEM((chunks, group, cap, width), normed.dtype),
            pltpu.SemaphoreType.DMA((chunks + 1, group)),
            pltpu.SemaphoreType.DMA((chunks + 1, group)),
            pltpu.SemaphoreType.DMA((chunks,)),
            pltpu.SemaphoreType.DMA((chunks,)),
            pltpu.SemaphoreType.DMA((chunks + 1,)),
        ],
        compiler_params=pltpu.CompilerParams(
            collective_id=2, has_side_effects=True, vmem_limit_bytes=40 * 2**20
        ),
    )(own_rows, normed, pick_far)


def collect_kernel(
    sp_half,
    dp_size,
    res_ref,
    high_ref,
    low_ref,
    o_ref,
    far_ref,
    landed,
    partial,
    send_sem,
    recv_sem,
    far_send,
    far_recv,
    own_sem,
):
    group = sp_half * dp_size
    chunks, _, cap, width = landed.shape
    here, mirror, peer = half_place(sp_half, dp_size)
    half_barrier(group, here, mirror, peer)

    def near(off):
        place = lax.rem(here + off, group)
        return pltpu.make_async_remote_copy(
            src_ref=res_ref.at[place],
            dst_ref=o_ref.at[here],
            send_sem=send_sem.at[chunks, off],
            recv_sem=recv_sem.at[chunks, off],
            device_id=peer(place),
            device_id_type=MESH,
        )

    def passed(chunk, off):
        place = lax.rem(here + off, group)
        return pltpu.make_async_remote_copy(
            src_ref=res_ref.at[group + place, :, pl.ds(chunk * width, width)],
            dst_ref=landed.at[chunk, here],
            send_sem=send_sem.at[chunk, off],
            recv_sem=recv_sem.at[chunk, off],
            device_id=peer(place),
            device_id_type=MESH,
        )

    def far(chunk):
        return pltpu.make_async_remote_copy(
            src_ref=partial.at[chunk],
            dst_ref=far_ref.at[:, pl.ds(chunk * width, width)],
            send_sem=far_send.at[chunk],
            recv_sem=far_recv.at[chunk],
            device_id=mirror,
            device_id_type=MESH,
        )

    def kept(chunk):
        return pltpu.make_async_copy(
            res_ref.at[group + here, :, pl.ds(chunk * width, width)],
            landed.at[chunk, here],
            own_sem.at[chunk],
        )

    def over(action):
        lax.fori_loop(1, group, lambda off, carry: (action(off), carry)[1], 0)

    for chunk in range(chunks):
        over(lambda off: passed(chunk, off).start())
        kept(chunk).start()
    over(lambda off: near(off).start())
    own = pltpu.make_async_copy(res_ref.at[here], o_ref.at[here], own_sem.at[chunks])
    own.start()
    contract = (((0,), (0,)), ((), ()))
    for chunk in range(chunks):
        kept(chunk).wait()
        over(lambda off: passed(chunk, off).wait_recv())
        block = landed[chunk].astype(jnp.float32).reshape(group * cap, width)
        block = block.astype(jnp.bfloat16)
        total = lax.dot_general(high_ref[...], block, contract, preferred_element_type=jnp.float32)
        total += lax.dot_general(low_ref[...], block, contract, preferred_element_type=jnp.float32)
        partial[chunk] = total.astype(partial.dtype)
        far(chunk).start()
    own.wait()
    over(lambda off: near(off).wait())
    for chunk in range(chunks):
        over(lambda off: passed(chunk, off).wait_send())
        far(chunk).wait()


def collect(sp_half, dp_size, results, high, low, chunks):
    twice, cap, model = results.shape
    group = twice // 2
    tok = high.shape[1]
    width = model // chunks
    return pl.pallas_call(
        functools.partial(collect_kernel, sp_half, dp_size),
        out_shape=[
            jax.ShapeDtypeStruct((group, cap, model), results.dtype),
            jax.ShapeDtypeStruct((tok, model), results.dtype),
        ],
        in_specs=[VMEM] * 3,
        out_specs=[VMEM] * 2,
        scratch_shapes=[
            pltpu.VMEM((chunks, group, cap, width), results.dtype),
            pltpu.VMEM((chunks, tok, width), results.dtype),
            pltpu.SemaphoreType.DMA((chunks + 1, group)),
            pltpu.SemaphoreType.DMA((chunks + 1, group)),
            pltpu.SemaphoreType.DMA((chunks,)),
            pltpu.SemaphoreType.DMA((chunks,)),
            pltpu.SemaphoreType.DMA((chunks + 1,)),
        ],
        compiler_params=pltpu.CompilerParams(
            collective_id=3, has_side_effects=True, vmem_limit_bytes=40 * 2**20
        ),
    )(results, high, low)


def slot_tables(chosen, weights, first, group, cap):
    tok = chosen.shape[0]
    ids = first + jnp.arange(group, dtype=jnp.int32)
    named = chosen.T[None] == ids[:, None, None]
    member = jnp.sum(named.astype(jnp.float32), axis=1)
    weight = jnp.sum(jnp.where(named, weights.T[None], 0.0), axis=1)
    before = jnp.arange(tok)[:, None] < jnp.arange(tok)[None, :]
    earlier = jnp.dot(
        member.astype(jnp.bfloat16),
        before.astype(jnp.bfloat16),
        preferred_element_type=jnp.float32,
    )
    rank = jnp.where(member > 0, earlier, -1.0)
    hit = rank[:, None, :] == jnp.arange(cap, dtype=jnp.float32)[None, :, None]
    spread = jnp.where(hit, weight[:, None, :], 0.0)
    high = spread.astype(jnp.bfloat16)
    low = (spread - high.astype(jnp.float32)).astype(jnp.bfloat16)
    flat = (group * cap, tok)
    return hit.astype(jnp.bfloat16).reshape(flat), high.reshape(flat), low.reshape(flat)


def local(
    queries,
    key_vectors,
    value_vectors,
    head_lambda,
    head_gain,
    residual,
    out_weight,
    mix_gain,
    pre_gain,
    post_gain,
    routes,
    route_weights,
    expert_gate,
    expert_up,
    expert_down,
    shared_gate,
    shared_up,
    shared_down,
):
    n, dp_size = lax.axis_size("sp"), lax.axis_size("dp")
    sp_half = n // 2
    group = sp_half * dp_size
    tok = queries.shape[1]
    top_count = routes.shape[2]
    cap = 3 * tok * top_count // (2 * n * dp_size)
    cap = (cap + 7) // 8 * 8
    model = residual.shape[2]
    chunks = 4

    sent = jnp.concatenate([routes[0].astype(jnp.float32), route_weights[0]], axis=1)
    far_sent = lax.ppermute(sent, "sp", [(i, (i + sp_half) % n) for i in range(n)])

    q, k, v = to_heads(
        n, queries.reshape(tok, -1), key_vectors.reshape(tok, -1), value_vectors.reshape(tok, -1)
    )
    width = q.shape[2]
    attended = attend(
        q.reshape(-1, width), k.reshape(-1, width), v.reshape(-1, width), head_lambda, head_gain
    )
    flat_heads = to_tokens(n, attended.reshape(n, tok, width))

    first = lax.axis_index("sp") // sp_half * group
    pick, high, low = slot_tables(routes[0], route_weights[0], first, group, cap)
    far_pick, far_high, far_low = slot_tables(
        far_sent[:, :top_count].astype(jnp.int32), far_sent[:, top_count:], first, group, cap
    )

    mixed_rows = jnp.dot(flat_heads, out_weight, preferred_element_type=jnp.float32)
    updated = (residual[0].astype(jnp.float32) + rms_scale(mixed_rows, mix_gain)).astype(
        jnp.bfloat16
    )
    normed = rms_scale(updated.astype(jnp.float32), pre_gain).astype(jnp.bfloat16)
    own_rows = jnp.dot(pick, normed, preferred_element_type=jnp.float32).astype(jnp.bfloat16)
    arrived = dispatch(
        sp_half, dp_size, own_rows.reshape(group, cap, model), normed, far_pick, chunks
    )
    shared_out = feed_forward(normed, shared_gate, shared_up, shared_down)
    results = feed_forward(
        arrived.reshape(-1, model), expert_gate[0], expert_up[0], expert_down[0]
    )
    returned, from_far = collect(
        sp_half, dp_size, results.reshape(2 * group, cap, model), far_high, far_low, chunks
    )
    rows = returned.reshape(group * cap, model)
    contract = (((0,), (0,)), ((), ()))
    routed = lax.dot_general(high, rows, contract, preferred_element_type=jnp.float32)
    routed += lax.dot_general(low, rows, contract, preferred_element_type=jnp.float32)
    combined = routed + from_far.astype(jnp.float32) + shared_out.astype(jnp.float32)
    output = (updated.astype(jnp.float32) + rms_scale(combined, post_gain)).astype(jnp.bfloat16)
    return output.reshape(1, tok, model)


def solution(mesh):
    in_specs = (
        P("dp", "sp", None, None),
        P("dp", "sp", None, None),
        P("dp", "sp", None, None),
        P("sp"),
        P(),
        P("dp", "sp", None),
        P(),
        P(),
        P(),
        P(),
        P("dp", "sp", None),
        P("dp", "sp", None),
        P(("sp", "dp"), None, None),
        P(("sp", "dp"), None, None),
        P(("sp", "dp"), None, None),
        P(),
        P(),
        P(),
    )
    out_specs = P("dp", "sp", None)
    return jax.shard_map(local, mesh=mesh, in_specs=in_specs, out_specs=out_specs, check_vma=False)
```

```python
import functools

import jax
import jax.numpy as jnp
from jax import lax
from jax.experimental import pallas as pl
from jax.experimental.pallas import tpu as pltpu
from jax.sharding import PartitionSpec as P

epsilon = 1e-06
MESH = pl.DeviceIdType.MESH
VMEM = pl.BlockSpec(memory_space=pltpu.VMEM)


def rms_scale(values_in, gain):
    return (
        values_in
        * lax.rsqrt(jnp.mean(values_in * values_in, axis=-1, keepdims=True) + epsilon)
        * gain
    )


def feed_forward(rows, gate_w, up_w, down_w):
    gate_val = jnp.dot(rows, gate_w, preferred_element_type=jnp.float32)
    up_val = jnp.dot(rows, up_w, preferred_element_type=jnp.float32)
    hidden = (jax.nn.silu(gate_val) * up_val).astype(jnp.bfloat16)
    return jnp.dot(hidden, down_w, preferred_element_type=jnp.float32).astype(jnp.bfloat16)


def columns_of(index, width):
    return pl.ds(pl.multiple_of(index * width, width), width)


def line_barrier(n, me):
    barrier = pltpu.get_barrier_semaphore()

    def greet(off, carry):
        pl.semaphore_signal(
            barrier, inc=1, device_id={"sp": lax.rem(me + off, n)}, device_id_type=MESH
        )
        return carry

    lax.fori_loop(1, n, greet, 0)
    pl.semaphore_wait(barrier, n - 1)


def to_heads_kernel(
    n,
    q_ref,
    k_ref,
    v_ref,
    side_ref,
    qo_ref,
    ko_ref,
    vo_ref,
    side_out,
    send_sem,
    recv_sem,
    own_sem,
    side_send,
    side_recv,
):
    me = lax.axis_index("sp")
    width = qo_ref.shape[2]
    pairs = ((q_ref, qo_ref), (k_ref, ko_ref), (v_ref, vo_ref))
    line_barrier(n, me)

    def copy(which, off):
        source, target = pairs[which]
        dst = lax.rem(me + off, n)
        return pltpu.make_async_remote_copy(
            src_ref=source.at[:, columns_of(dst, width)],
            dst_ref=target.at[me],
            send_sem=send_sem.at[which, off],
            recv_sem=recv_sem.at[which, off],
            device_id={"sp": dst},
            device_id_type=MESH,
        )

    def own(which):
        source, target = pairs[which]
        return pltpu.make_async_copy(
            source.at[:, columns_of(me, width)], target.at[me], own_sem.at[which]
        )

    def start(off, carry):
        for which in range(3):
            copy(which, off).start()
        return carry

    def finish(off, carry):
        for which in range(3):
            copy(which, off).wait()
        return carry

    side = pltpu.make_async_remote_copy(
        src_ref=side_ref,
        dst_ref=side_out,
        send_sem=side_send,
        recv_sem=side_recv,
        device_id={"sp": lax.rem(me + n // 2, n)},
        device_id_type=MESH,
    )
    lax.fori_loop(1, n, start, 0)
    side.start()
    for which in range(3):
        own(which).start()
    for which in range(3):
        own(which).wait()
    lax.fori_loop(1, n, finish, 0)
    side.wait()


def to_heads(n, q, k, v, side):
    tok, model = q.shape
    width = model // n
    out = jax.ShapeDtypeStruct((n, tok, width), q.dtype)
    return pl.pallas_call(
        functools.partial(to_heads_kernel, n),
        out_shape=[out] * 3 + [jax.ShapeDtypeStruct(side.shape, side.dtype)],
        in_specs=[VMEM] * 4,
        out_specs=[VMEM] * 4,
        scratch_shapes=[
            pltpu.SemaphoreType.DMA((3, n)),
            pltpu.SemaphoreType.DMA((3, n)),
            pltpu.SemaphoreType.DMA((3,)),
            pltpu.SemaphoreType.DMA,
            pltpu.SemaphoreType.DMA,
        ],
        compiler_params=pltpu.CompilerParams(
            collective_id=0, has_side_effects=True, vmem_limit_bytes=32 * 2**20
        ),
    )(q, k, v, side)


def to_tokens_kernel(n, a_ref, o_ref, send_sem, recv_sem, own_sem):
    me = lax.axis_index("sp")
    width = a_ref.shape[2]
    line_barrier(n, me)

    def copy(off):
        dst = lax.rem(me + off, n)
        return pltpu.make_async_remote_copy(
            src_ref=a_ref.at[dst],
            dst_ref=o_ref.at[:, columns_of(me, width)],
            send_sem=send_sem.at[off],
            recv_sem=recv_sem.at[off],
            device_id={"sp": dst},
            device_id_type=MESH,
        )

    def start(off, carry):
        copy(off).start()
        return carry

    def finish(off, carry):
        copy(off).wait()
        return carry

    lax.fori_loop(1, n, start, 0)
    own = pltpu.make_async_copy(a_ref.at[me], o_ref.at[:, columns_of(me, width)], own_sem)
    own.start()
    own.wait()
    lax.fori_loop(1, n, finish, 0)


def to_tokens(n, attended):
    _, tok, width = attended.shape
    return pl.pallas_call(
        functools.partial(to_tokens_kernel, n),
        out_shape=jax.ShapeDtypeStruct((tok, n * width), attended.dtype),
        in_specs=[VMEM],
        out_specs=VMEM,
        scratch_shapes=[
            pltpu.SemaphoreType.DMA((n,)),
            pltpu.SemaphoreType.DMA((n,)),
            pltpu.SemaphoreType.DMA,
        ],
        compiler_params=pltpu.CompilerParams(
            collective_id=1, has_side_effects=True, vmem_limit_bytes=32 * 2**20
        ),
    )(attended)


def attend_kernel(block, q_ref, k_ref, v_ref, lam_ref, gain_ref, o_ref):
    length, width = q_ref.shape
    value_size = gain_ref.shape[1]
    heads = width // value_size
    half = value_size // 2
    lane = lax.broadcasted_iota(jnp.int32, (block, value_size), 1)
    row = lax.broadcasted_iota(jnp.int32, (block, block), 0)
    col = lax.broadcasted_iota(jnp.int32, (block, block), 1)
    causal = col <= row
    contract = (((1,), (1,)), ((), ()))
    for head in range(heads):
        cols = slice(head * value_size, (head + 1) * value_size)
        for step in range(length // block):
            rows = slice(step * block, (step + 1) * block)
            past = step * block
            query = q_ref[rows, cols]
            near, far = [], []
            for which in range(2):
                keep = (lane < half) if which == 0 else (lane >= half)
                part = jnp.where(keep, query, jnp.zeros_like(query))
                s_near = lax.dot_general(
                    part, k_ref[rows, cols], contract, preferred_element_type=jnp.float32
                ) * (half**-0.5)
                s_near = jnp.where(causal, s_near, -jnp.inf)
                top = jnp.max(s_near, axis=-1, keepdims=True)
                if past:
                    s_far = lax.dot_general(
                        part, k_ref[:past, cols], contract, preferred_element_type=jnp.float32
                    ) * (half**-0.5)
                    top = jnp.maximum(top, jnp.max(s_far, axis=-1, keepdims=True))
                e_near = jnp.exp(s_near - top)
                total = jnp.sum(e_near, axis=-1, keepdims=True)
                if past:
                    e_far = jnp.exp(s_far - top)
                    total = total + jnp.sum(e_far, axis=-1, keepdims=True)
                scale = 1.0 / total
                if which == 1:
                    scale = scale * lam_ref[head]
                near.append(e_near * scale)
                if past:
                    far.append(e_far * scale)
            mixture = (near[0] - near[1]).astype(jnp.bfloat16)
            result = jnp.dot(mixture, v_ref[rows, cols], preferred_element_type=jnp.float32)
            if past:
                mixture = (far[0] - far[1]).astype(jnp.bfloat16)
                result += jnp.dot(
                    mixture, v_ref[:past, cols], preferred_element_type=jnp.float32
                )
            o_ref[rows, cols] = rms_scale(result, gain_ref[...]).astype(o_ref.dtype)


def attend(q, k, v, head_lambda, head_gain):
    return pl.pallas_call(
        functools.partial(attend_kernel, min(256, q.shape[0])),
        out_shape=jax.ShapeDtypeStruct(q.shape, q.dtype),
        in_specs=[VMEM] * 3 + [pl.BlockSpec(memory_space=pltpu.SMEM), VMEM],
        out_specs=VMEM,
        compiler_params=pltpu.CompilerParams(vmem_limit_bytes=48 * 2**20),
    )(q, k, v, head_lambda, head_gain.reshape(1, -1))


def half_place(sp_half, dp_size):
    sp, dp = lax.axis_index("sp"), lax.axis_index("dp")
    first = sp // sp_half * sp_half
    here = (sp - first) * dp_size + dp
    mirror = {"sp": lax.rem(sp + sp_half, 2 * sp_half), "dp": dp}

    def peer(place):
        return {"sp": first + place // dp_size, "dp": lax.rem(place, dp_size)}

    return here, mirror, peer


def half_barrier(group, here, mirror, peer):
    barrier = pltpu.get_barrier_semaphore()
    pl.semaphore_signal(barrier, inc=1, device_id=mirror, device_id_type=MESH)

    def greet(off, carry):
        pl.semaphore_signal(
            barrier, inc=1, device_id=peer(lax.rem(here + off, group)), device_id_type=MESH
        )
        return carry

    lax.fori_loop(1, group, greet, 0)
    pl.semaphore_wait(barrier, group)


def experts_kernel(
    sp_half,
    dp_size,
    normed_ref,
    own_pick_ref,
    far_pick_ref,
    high_ref,
    low_ref,
    gate_hbm,
    up_hbm,
    down_hbm,
    o_ref,
    far_ref,
    gate_w,
    up_w,
    down_w,
    own_rows,
    tokens,
    rows,
    own_in,
    far_in,
    flat,
    hidden,
    own_out,
    far_out,
    landed,
    partial,
    send_sem,
    recv_sem,
    back_send,
    back_recv,
    far_send,
    far_recv,
    local_sem,
):
    group = sp_half * dp_size
    chunks, _, cap, width = rows.shape
    here, mirror, peer = half_place(sp_half, dp_size)
    half_barrier(group, here, mirror, peer)

    def cols(chunk):
        return pl.ds(chunk * width, width)

    def far(way, chunk):
        return pltpu.make_async_remote_copy(
            src_ref=(partial.at[chunk] if way else normed_ref.at[:, cols(chunk)]),
            dst_ref=(far_ref.at[:, cols(chunk)] if way else tokens.at[chunk]),
            send_sem=far_send.at[way, chunk],
            recv_sem=far_recv.at[way, chunk],
            device_id=mirror,
            device_id_type=MESH,
        )

    def send(off, source, target, row, sends, recvs):
        place = lax.rem(here + off, group)
        return pltpu.make_async_remote_copy(
            src_ref=source(place),
            dst_ref=target(here),
            send_sem=sends.at[row, off],
            recv_sem=recvs.at[row, off],
            device_id=peer(place),
            device_id_type=MESH,
        )

    def keep(source, target, index):
        return pltpu.make_async_copy(source(here), target(here), local_sem.at[index])

    def over(action):
        lax.fori_loop(1, group, lambda off, carry: (action(off), carry)[1], 0)

    out_own = (lambda p: own_rows.at[p], lambda p: own_in.at[p])
    back_own = (lambda p: own_out.at[p], lambda p: o_ref.at[p])

    def out_far(chunk):
        return (lambda p: rows.at[chunk, p], lambda p: far_in.at[p, :, cols(chunk)])

    def back_far(chunk):
        return (lambda p: far_out.at[p, :, cols(chunk)], lambda p: landed.at[chunk, p])

    def near(off):
        return send(off, *out_own, chunks, send_sem, recv_sem)

    def passed(chunk, off):
        return send(off, *out_far(chunk), chunk, send_sem, recv_sem)

    def near_back(off):
        return send(off, *back_own, chunks, back_send, back_recv)

    def passed_back(chunk, off):
        return send(off, *back_far(chunk), chunk, back_send, back_recv)

    loads = [
        pltpu.make_async_copy(source, target, local_sem.at[2 * chunks + 2 + index])
        for index, (source, target) in enumerate(
            ((gate_hbm, gate_w), (up_hbm, up_w), (down_hbm, down_w))
        )
    ]
    tile = min(256, gate_w.shape[1])

    def hidden_of(block):
        for chunk in range(chunks):
            part = block[:, :, chunk * width : (chunk + 1) * width].astype(jnp.float32)
            flat[:, chunk * width : (chunk + 1) * width] = part.reshape(
                group * cap, width
            ).astype(flat.dtype)

        def one(index, carry):
            some = columns_of(index, tile)
            gate_val = jnp.dot(flat[...], gate_w[:, some], preferred_element_type=jnp.float32)
            up_val = jnp.dot(flat[...], up_w[:, some], preferred_element_type=jnp.float32)
            hidden[:, some] = (jax.nn.silu(gate_val) * up_val).astype(hidden.dtype)
            return carry

        lax.fori_loop(0, gate_w.shape[1] // tile, one, 0)

    def down_to(target, chunk):
        part = slice(chunk * width, (chunk + 1) * width)
        value = jnp.dot(hidden[...], down_w[:, part], preferred_element_type=jnp.float32)
        target[:, :, part] = value.reshape(group, cap, width).astype(target.dtype)

    for chunk in range(chunks):
        far(0, chunk).start()
    for chunk in range(chunks):
        part = slice(chunk * width, (chunk + 1) * width)
        value = jnp.dot(
            own_pick_ref[...], normed_ref[:, part], preferred_element_type=jnp.float32
        )
        own_rows[:, :, part] = value.reshape(group, cap, width).astype(own_rows.dtype)
    over(lambda off: near(off).start())
    keep(*out_own, 2 * chunks).start()
    for load in loads:
        load.start()
    for chunk in range(chunks):
        far(0, chunk).wait_recv()
        picked = jnp.dot(far_pick_ref[...], tokens[chunk], preferred_element_type=jnp.float32)
        rows[chunk] = picked.reshape(rows.shape[1:]).astype(rows.dtype)
        over(lambda off: passed(chunk, off).start())
        keep(*out_far(chunk), chunk).start()

    for load in loads:
        load.wait()
    keep(*out_own, 2 * chunks).wait()
    over(lambda off: near(off).wait_recv())
    hidden_of(own_in)
    for chunk in range(chunks):
        down_to(own_out, chunk)
    over(lambda off: near_back(off).start())
    keep(*back_own, 2 * chunks + 1).start()

    for chunk in range(chunks):
        keep(*out_far(chunk), chunk).wait()
        over(lambda off: passed(chunk, off).wait_recv())
    hidden_of(far_in)
    for chunk in range(chunks):
        down_to(far_out, chunk)
        over(lambda off: passed_back(chunk, off).start())
        keep(*back_far(chunk), chunks + chunk).start()

    contract = (((0,), (0,)), ((), ()))
    for chunk in range(chunks):
        keep(*back_far(chunk), chunks + chunk).wait()
        over(lambda off: passed_back(chunk, off).wait_recv())
        block = landed[chunk].astype(jnp.float32).reshape(group * cap, width)
        block = block.astype(jnp.bfloat16)
        total = lax.dot_general(high_ref[...], block, contract, preferred_element_type=jnp.float32)
        total += lax.dot_general(low_ref[...], block, contract, preferred_element_type=jnp.float32)
        partial[chunk] = total.astype(partial.dtype)
        far(1, chunk).start()

    keep(*back_own, 2 * chunks + 1).wait()
    over(lambda off: near(off).wait_send())
    over(lambda off: near_back(off).wait())
    for chunk in range(chunks):
        over(lambda off: passed(chunk, off).wait_send())
        over(lambda off: passed_back(chunk, off).wait_send())
        far(0, chunk).wait_send()
        far(1, chunk).wait()


def run_experts(sp_half, dp_size, cap, chunks, normed, picks, parts, gate, up, down):
    group = sp_half * dp_size
    tok, model = normed.shape
    ff = gate.shape[1]
    width = model // chunks
    kind = normed.dtype
    whole = pltpu.VMEM((group, cap, model), kind)
    pieces = pltpu.VMEM((chunks, group, cap, width), kind)
    token_pieces = pltpu.VMEM((chunks, tok, width), kind)
    return pl.pallas_call(
        functools.partial(experts_kernel, sp_half, dp_size),
        out_shape=[
            jax.ShapeDtypeStruct((group, cap, model), kind),
            jax.ShapeDtypeStruct((tok, model), kind),
        ],
        in_specs=[VMEM] * 5 + [pl.BlockSpec(memory_space=pl.ANY)] * 3,
        out_specs=[VMEM] * 2,
        scratch_shapes=[
            pltpu.VMEM((model, ff), kind),
            pltpu.VMEM((model, ff), kind),
            pltpu.VMEM((ff, model), kind),
            whole,
            token_pieces,
            pieces,
            whole,
            whole,
            pltpu.VMEM((group * cap, model), kind),
            pltpu.VMEM((group * cap, ff), kind),
            whole,
            whole,
            pieces,
            token_pieces,
        ]
        + [pltpu.SemaphoreType.DMA((chunks + 1, group))] * 4
        + [pltpu.SemaphoreType.DMA((2, chunks))] * 2
        + [pltpu.SemaphoreType.DMA((2 * chunks + 5,))],
        compiler_params=pltpu.CompilerParams(
            collective_id=2, has_side_effects=True, vmem_limit_bytes=56 * 2**20
        ),
    )(normed, *picks, *parts, gate, up, down)


def slot_tables(chosen, weights, first, group, cap):
    tok = chosen.shape[0]
    ids = first + jnp.arange(group, dtype=jnp.int32)
    named = chosen.T[None] == ids[:, None, None]
    member = jnp.sum(named.astype(jnp.float32), axis=1)
    weight = jnp.sum(jnp.where(named, weights.T[None], 0.0), axis=1)
    before = jnp.arange(tok)[:, None] < jnp.arange(tok)[None, :]
    earlier = jnp.dot(
        member.astype(jnp.bfloat16),
        before.astype(jnp.bfloat16),
        preferred_element_type=jnp.float32,
    )
    rank = jnp.where(member > 0, earlier, -1.0)
    hit = rank[:, None, :] == jnp.arange(cap, dtype=jnp.float32)[None, :, None]
    spread = jnp.where(hit, weight[:, None, :], 0.0)
    high = spread.astype(jnp.bfloat16)
    low = (spread - high.astype(jnp.float32)).astype(jnp.bfloat16)
    flat = (group * cap, tok)
    return hit.astype(jnp.bfloat16).reshape(flat), high.reshape(flat), low.reshape(flat)


def local(
    queries,
    key_vectors,
    value_vectors,
    head_lambda,
    head_gain,
    residual,
    out_weight,
    mix_gain,
    pre_gain,
    post_gain,
    routes,
    route_weights,
    expert_gate,
    expert_up,
    expert_down,
    shared_gate,
    shared_up,
    shared_down,
):
    n, dp_size = lax.axis_size("sp"), lax.axis_size("dp")
    sp_half = n // 2
    group = sp_half * dp_size
    tok = queries.shape[1]
    top_count = routes.shape[2]
    cap = 3 * tok * top_count // (2 * n * dp_size)
    cap = (cap + 7) // 8 * 8
    model = residual.shape[2]
    chunks = 4

    sent = jnp.concatenate([routes[0].astype(jnp.float32), route_weights[0]], axis=1)
    sent = jnp.pad(sent, ((0, 0), (0, 128 - 2 * top_count)))

    q, k, v, far_sent = to_heads(
        n,
        queries.reshape(tok, -1),
        key_vectors.reshape(tok, -1),
        value_vectors.reshape(tok, -1),
        sent,
    )
    width = q.shape[2]
    attended = attend(
        q.reshape(-1, width), k.reshape(-1, width), v.reshape(-1, width), head_lambda, head_gain
    )
    flat_heads = to_tokens(n, attended.reshape(n, tok, width))

    first = lax.axis_index("sp") // sp_half * group
    pick, high, low = slot_tables(routes[0], route_weights[0], first, group, cap)
    far_pick, far_high, far_low = slot_tables(
        far_sent[:, :top_count].astype(jnp.int32), far_sent[:, top_count : 2 * top_count], first, group, cap
    )

    mixed_rows = jnp.dot(flat_heads, out_weight, preferred_element_type=jnp.float32)
    updated = (residual[0].astype(jnp.float32) + rms_scale(mixed_rows, mix_gain)).astype(
        jnp.bfloat16
    )
    normed = rms_scale(updated.astype(jnp.float32), pre_gain).astype(jnp.bfloat16)
    returned, from_far = run_experts(
        sp_half,
        dp_size,
        cap,
        chunks,
        normed,
        (pick, far_pick),
        (far_high, far_low),
        expert_gate[0],
        expert_up[0],
        expert_down[0],
    )
    shared_out = feed_forward(normed, shared_gate, shared_up, shared_down)
    rows = returned.reshape(group * cap, model)
    contract = (((0,), (0,)), ((), ()))
    routed = lax.dot_general(high, rows, contract, preferred_element_type=jnp.float32)
    routed += lax.dot_general(low, rows, contract, preferred_element_type=jnp.float32)
    combined = routed + from_far.astype(jnp.float32) + shared_out.astype(jnp.float32)
    output = (updated.astype(jnp.float32) + rms_scale(combined, post_gain)).astype(jnp.bfloat16)
    return output.reshape(1, tok, model)


def solution(mesh):
    in_specs = (
        P("dp", "sp", None, None),
        P("dp", "sp", None, None),
        P("dp", "sp", None, None),
        P("sp"),
        P(),
        P("dp", "sp", None),
        P(),
        P(),
        P(),
        P(),
        P("dp", "sp", None),
        P("dp", "sp", None),
        P(("sp", "dp"), None, None),
        P(("sp", "dp"), None, None),
        P(("sp", "dp"), None, None),
        P(),
        P(),
        P(),
    )
    out_specs = P("dp", "sp", None)
    return jax.shard_map(local, mesh=mesh, in_specs=in_specs, out_specs=out_specs, check_vma=False)
```
